32 devices in a mesh: grp: 2 (over y), dp: 2 (over x), kv: 4 (over z), tp: 2 (over core).
Axes of the slice: x: 2, y: 2, z: 4, core: 2. Of those that a mesh axis runs over, the one named last changes fastest.
Arguments:
- resid: bfloat16 [12, 2048], P(('grp', 'dp'), ('kv', 'tp')), parts along dimension 0, may hold values from -7 to 7
- keys_cache: bfloat16 [12, 4096, 256], P(('grp', 'dp'), 'kv', 'tp'), parts along dimension 0, may hold values from -310 to 310
- values_cache: bfloat16 [12, 4096, 256], P(('grp', 'dp'), 'kv', 'tp'), parts along dimension 0, may hold values from -6 to 6
- gates_cache: float32 [12, 4096, 4], P(('grp', 'dp'), 'kv', 'tp'), parts along dimension 0, may hold values from -1044 to 0, as said below
- norm_gain: float32 [2048], replicated, may hold values from 0.1 to 1.9
- w_query: bfloat16 [2048, 2048], P('kv', 'tp'), may hold values from -0.125 to 0.125
- w_key: bfloat16 [2048, 256], P('kv', 'tp'), may hold values from -0.125 to 0.125
- w_value: bfloat16 [2048, 256], P('kv', 'tp'), may hold values from -0.5 to 0.5
- w_forget: bfloat16 [2048, 4], replicated, may hold values from -0.125 to 0.125
- forget_bias: float32 [4], replicated, may hold values from -3 to 1
- w_out: bfloat16 [2048, 2048], P('tp', 'kv'), may hold values from -0.5 to 0.5
- mlp_gain: float32 [2048], replicated, may hold values from 0.1 to 1.9
- w_up: bfloat16 [2048, 8192], P('kv', 'tp'), may hold values from -0.125 to 0.125
- w_down: bfloat16 [8192, 2048], P('tp', 'kv'), may hold values from -0.0625 to 0.0625
Outputs:
- next_resid: bfloat16 [12, 2048], P(('grp', 'dp'), ('kv', 'tp')), parts along dimension 0
The draws below stay inside these ranges and needn't reach their ends.
There are 2 independent parts, one for each index of `grp`. The reference program is written for one: setup_inputs(seed, part) draws one part's arguments, and reference() takes and returns one part's arrays. A program takes and returns all parts, laid end to end along the dimension named above; an argument that names none is the same for every part. Nothing has to cross between parts.
Inputs may be any that keep to these rules, and one draw needn't show every extreme that they name: gates_cache[b, p, g] is the sum of the log forget gates of the cached positions after p, so it never falls along the positions and is 0 at the last one.
All inputs are finite; a program needn't handle non-finite values.
Results may differ from the reference program's by a relative error of at most 0.028.
Values may be sent and summed in bfloat16 or wider, within the bound.
A program may use at most 64 MiB of HBM per device.

```python
import jax
import jax.numpy as jnp
from jax import lax

D = 2048
HEADS = 32
LOOKUP_GROUPS = 4
HEAD = 64
FF = 8192
CTX_DEV = 1024
TOTAL_STRINGS = 6
STORED_SLOTS = 4096
QW = 2048
KW = 256
N_TP = 2


def draw_resid(key, part):
    key_base, key_cols, key_rows = jax.random.split(jax.random.fold_in(key, 5), 3)
    columns = jnp.arange(D, dtype=jnp.float32) / D
    col_scale = jnp.exp(jnp.log(0.1) + jnp.log(5.0) * columns + 0.3 * jax.random.uniform(key_cols, (D,), jnp.float32, -1.0, 1.0))
    base = jnp.clip(jax.random.normal(key_base, (TOTAL_STRINGS, D), jnp.float32), -5.0, 5.0)
    row_scale = jnp.exp(jax.random.uniform(key_rows, (TOTAL_STRINGS, 1), jnp.float32, 0.0, jnp.log(2.0)))
    return (base * col_scale * row_scale).astype(jnp.bfloat16)


def draw_keys_cache(key, part):
    key_base = jax.random.fold_in(jax.random.fold_in(key, 3), 0)
    keys = jnp.clip(jax.random.normal(key_base, (TOTAL_STRINGS, STORED_SLOTS, KW), jnp.float32), -5.0, 5.0)
    return keys.astype(jnp.bfloat16)


def draw_gates_cache(key, part):
    seed_gradual, seed_speed, seed_quick, seed_tile, seed_jitter, seed_spike, seed_discard = jax.random.split(jax.random.fold_in(key, 9), 7)
    pick = jax.random.uniform(seed_gradual, (TOTAL_STRINGS, 1, LOOKUP_GROUPS), jnp.float32)
    slow = pick < 0.5
    slow_rate = jax.random.uniform(seed_speed, (TOTAL_STRINGS, 1, LOOKUP_GROUPS), jnp.float32, 0.3, 1.0) / STORED_SLOTS
    fast_rate = 1.0 / jax.random.uniform(seed_quick, (TOTAL_STRINGS, 1, LOOKUP_GROUPS), jnp.float32, 25.0, 60.0)
    rate = jnp.where(slow, slow_rate, fast_rate)
    factor = jnp.exp(jax.random.uniform(seed_tile, (TOTAL_STRINGS, STORED_SLOTS // CTX_DEV, LOOKUP_GROUPS), jnp.float32, jnp.log(0.5), jnp.log(2.0)))
    factor = jnp.repeat(factor, CTX_DEV, axis=1)
    noise = jax.random.uniform(seed_jitter, (TOTAL_STRINGS, STORED_SLOTS, LOOKUP_GROUPS), jnp.float32, 0.5, 1.5)
    log_increments = -rate * factor * noise
    spike_magnitude = jax.random.uniform(seed_spike, (TOTAL_STRINGS, STORED_SLOTS, LOOKUP_GROUPS), jnp.float32) < 2.0 / STORED_SLOTS
    discard_proportion = jnp.log(jax.random.uniform(seed_discard, (TOTAL_STRINGS, STORED_SLOTS, LOOKUP_GROUPS), jnp.float32, 0.5, 0.8))
    log_increments = log_increments + jnp.where(spike_magnitude, discard_proportion, 0.0)
    after = jnp.flip(jnp.cumsum(jnp.flip(log_increments, 1), 1), 1) - log_increments
    return after


def shard_levels(own_key, dims, cuts, least, top_value):
    factor_of, own = 1.0, jax.random.fold_in(own_key, 6)
    for position, blocks in cuts:
        heights = jnp.exp(jax.random.uniform(jax.random.fold_in(own, position), (blocks,), jnp.float32, least / len(cuts), top_value / len(cuts)))
        factor_of = factor_of * jnp.repeat(heights, dims[position] // blocks).reshape([-1 if axis == position else 1 for axis in range(len(dims))])
    return factor_of


def scatter_about(own_key, extent, scale, bound, cuts=(), held_as=jnp.bfloat16):
    result = scale * jax.random.normal(own_key, extent, jnp.float32)
    if cuts:
        result = result * shard_levels(own_key, extent, cuts, -0.22, 0.18)
    return jnp.clip(result, -bound, bound).astype(held_as)


def setup_inputs(seed: int = 0, part: int = 0) -> dict:
    splits = jax.random.split(jax.random.key(seed), 15)
    part_splits = jax.random.split(jax.random.fold_in(splits[14], part), 15)
    resid = draw_resid(jax.random.fold_in(jax.random.fold_in(splits[14], part), 71), part)
    keys_cache = draw_keys_cache(jax.random.fold_in(jax.random.fold_in(splits[14], part), 71), part)
    values_cache = scatter_about(part_splits[2], (TOTAL_STRINGS, STORED_SLOTS, KW), 1.0, 6.0, ((0, 2), (1, 4), (2, 2)))
    gates_cache = draw_gates_cache(jax.random.fold_in(jax.random.fold_in(splits[14], part), 71), part)
    norm_gain = jnp.clip(1.0 + 0.18 * jax.random.normal(splits[4], (D,), jnp.float32), 0.1, 1.9)
    w_query = scatter_about(splits[5], (D, QW), D ** -0.5, 0.125, ((0, 4), (1, 2)))
    w_key = scatter_about(splits[6], (D, KW), D ** -0.5, 0.125, ((0, 4), (1, 2)))
    w_value = scatter_about(splits[7], (D, KW), (D // 16) ** -0.5, 0.5, ((0, 4), (1, 2)))
    w_forget = scatter_about(splits[8], (D, LOOKUP_GROUPS), D ** -0.5, 0.125)
    forget_bias = jnp.clip(jax.random.uniform(splits[9], (LOOKUP_GROUPS,), jnp.float32, -3.0, 1.0), -3.0, 1.0)
    w_out = scatter_about(splits[10], (QW, D), (QW // 16) ** -0.5, 0.5, ((0, 2), (1, 4)))
    mlp_gain = jnp.clip(1.0 + 0.18 * jax.random.normal(splits[11], (D,), jnp.float32), 0.1, 1.9)
    w_up = scatter_about(splits[12], (D, FF), D ** -0.5, 0.125, ((0, 4), (1, 2)))
    w_down = scatter_about(splits[13], (FF, D), FF ** -0.5, 0.0625, ((0, 2), (1, 4)))
    return {"resid": resid, "keys_cache": keys_cache, "values_cache": values_cache, "gates_cache": gates_cache, "norm_gain": norm_gain, "w_query": w_query, "w_key": w_key, "w_value": w_value, "w_forget": w_forget, "forget_bias": forget_bias, "w_out": w_out, "mlp_gain": mlp_gain, "w_up": w_up, "w_down": w_down}


EPS = 1e-06

def scaled_rows(source, gain_vector):
    values32 = source.astype(jnp.float32)
    inverse = lax.rsqrt(lax.optimization_barrier(jnp.mean(values32 * values32, axis=1, keepdims=True)) + EPS)
    scaled = (values32 * gain_vector).astype(jnp.bfloat16)
    return (scaled, inverse)

def attend_sequence(inputs):
    query, key_new, value_new, log_forget, cached_keys, cached_values, cached_gates = inputs
    group_size = HEADS // LOOKUP_GROUPS
    score_scale = HEAD ** (-0.5)
    query32 = query.astype(jnp.float32).reshape(LOOKUP_GROUPS, group_size, HEAD)
    keys32 = cached_keys.astype(jnp.float32).reshape(STORED_SLOTS, LOOKUP_GROUPS, HEAD)
    values32 = cached_values.astype(jnp.float32).reshape(STORED_SLOTS, LOOKUP_GROUPS, HEAD)
    scores = jnp.einsum('gjd,pgd->gjp', query32, keys32) * score_scale
    scores = scores + (jnp.transpose(cached_gates) + log_forget[:, None])[:, None, :]
    fresh = jnp.einsum('gjd,gd->gj', query32, key_new.astype(jnp.float32).reshape(LOOKUP_GROUPS, HEAD)) * score_scale
    new_peak = jnp.maximum(lax.optimization_barrier(jnp.max(scores, axis=2)), fresh)
    weights = jnp.exp(scores - new_peak[:, :, None])
    own_weight = jnp.exp(fresh - new_peak)
    totals = lax.optimization_barrier(jnp.sum(weights, axis=2)) + own_weight
    rounded = lax.optimization_barrier(weights.astype(jnp.bfloat16)).astype(jnp.float32)
    own_rounded = lax.optimization_barrier(own_weight.astype(jnp.bfloat16)).astype(jnp.float32)
    mixed = jnp.einsum('gjp,pgd->gjd', rounded, values32)
    mixed = mixed + own_rounded[:, :, None] * value_new.astype(jnp.float32).reshape(LOOKUP_GROUPS, 1, HEAD)
    return (mixed / totals[:, :, None]).astype(jnp.bfloat16).reshape(HEADS * HEAD)

def split_product(left, right, pieces):
    width_piece = left.shape[1] // pieces
    total = jnp.zeros((left.shape[0], right.shape[1]), jnp.float32)
    for shard_index in range(pieces):
        lower = shard_index * width_piece
        part = jnp.dot(left[:, lower:lower + width_piece], right[lower:lower + width_piece], preferred_element_type=jnp.float32)
        total = total + part.astype(jnp.bfloat16).astype(jnp.float32)
    return total

def reference(resid, keys_cache, values_cache, gates_cache, norm_gain, w_query, w_key, w_value, w_forget, forget_bias, w_out, mlp_gain, w_up, w_down):
    scaled, inverse = scaled_rows(resid, norm_gain)
    query = (jnp.dot(scaled, w_query, preferred_element_type=jnp.float32) * inverse).astype(jnp.bfloat16)
    key_new = (jnp.dot(scaled, w_key, preferred_element_type=jnp.float32) * inverse).astype(jnp.bfloat16)
    value_new = (jnp.dot(scaled, w_value, preferred_element_type=jnp.float32) * inverse).astype(jnp.bfloat16)
    log_forget = jax.nn.log_sigmoid(jnp.dot(scaled, w_forget, preferred_element_type=jnp.float32) * inverse + forget_bias)
    attended = lax.map(attend_sequence, (query, key_new, value_new, log_forget, keys_cache, values_cache, gates_cache))
    middle = (resid.astype(jnp.float32) + split_product(attended, w_out, N_TP)).astype(jnp.bfloat16)
    scaled_mid, inverse_mid = scaled_rows(middle, mlp_gain)
    up_total = jnp.dot(scaled_mid, w_up, preferred_element_type=jnp.float32) * inverse_mid
    hidden = jnp.square(jax.nn.relu(up_total)).astype(jnp.bfloat16)
    return (middle.astype(jnp.float32) + split_product(hidden, w_down, N_TP)).astype(jnp.bfloat16)
```

```python
import functools

import jax
import jax.numpy as jnp
from jax import lax
from jax.experimental import pallas as pl
from jax.experimental.pallas import tpu as pltpu
from jax.sharding import PartitionSpec as P

HEADS = 32
LOOKUP_GROUPS = 4
HEAD = 64
EPS = 1e-06
CHUNKS = 4
MESH = pl.DeviceIdType.MESH
F32 = jnp.float32
BF16 = jnp.bfloat16


def layer_kernel(
    n_kv,
    n_tp,
    resid,
    keys,
    values,
    gates,
    gain1,
    w_query,
    w_key,
    w_value,
    w_forget_t,
    bias,
    w_out,
    gain2,
    w_up,
    w_down,
    out,
    halves,
    gain1_v,
    wqkv,
    wf_v,
    bias_v,
    keys_v,
    values_v,
    gates_v,
    wo_v,
    gain2_v,
    wu_v,
    wd_v,
    proj,
    qs,
    soft,
    att,
    branch,
    norm2,
    ups,
    tail_out,
    tail_in,
    load_sem,
    tp_send,
    tp_recv,
    kv_send,
    kv_recv,
):
    kv = lax.axis_index("kv")
    tp = lax.axis_index("tp")
    peer = lax.rem(tp + 1, n_tp)
    rows, half = resid.shape
    width = half * n_tp
    features = width * n_kv
    qw = w_query.shape[1]
    kw = w_key.shape[1]
    local_heads = kw // HEAD
    group = HEADS // LOOKUP_GROUPS
    ff = w_up.shape[1]
    ff_chunk = ff // CHUNKS

    def load(index, source, target):
        copy = pltpu.make_async_copy(source, target, load_sem.at[index])
        copy.start()
        return copy

    load_resid = load(0, resid, halves.at[tp])
    load_gain1 = load(1, gain1, gain1_v)
    load_wq = load(2, w_query, wqkv.at[:, pl.ds(0, qw)])
    load_wk = load(3, w_key, wqkv.at[:, pl.ds(qw, kw)])
    load_wv = load(4, w_value, wqkv.at[:, pl.ds(qw + kw, kw)])
    load_wf = load(5, w_forget_t, wf_v)
    load_bias = load(6, bias, bias_v)

    barrier = pltpu.get_barrier_semaphore()
    pl.semaphore_signal(barrier, inc=1, device_id={"tp": peer}, device_id_type=MESH)
    for step in range(1, n_kv):
        pl.semaphore_signal(
            barrier, inc=1, device_id={"kv": lax.rem(kv + step, n_kv)}, device_id_type=MESH
        )
    load_keys = load(7, keys, keys_v)
    load_gates = load(8, gates, gates_v)
    load_values = load(9, values, values_v)
    load_wo = load(10, w_out, wo_v)
    load_gain2 = load(11, gain2, gain2_v)
    load_wu = load(12, w_up, wu_v)
    load_wd = load(13, w_down, wd_v)
    sends = []

    def to_peer(index, source, target):
        copy = pltpu.make_async_remote_copy(
            src_ref=source,
            dst_ref=target,
            send_sem=tp_send.at[index],
            recv_sem=tp_recv.at[index],
            device_id={"tp": peer},
            device_id_type=MESH,
        )
        copy.start()
        sends.append(copy)
        return copy

    def to_all(index, block):
        copies = []
        for step in range(1, n_kv):
            slot = index * (n_kv - 1) + step - 1
            copy = pltpu.make_async_remote_copy(
                src_ref=block,
                dst_ref=block,
                send_sem=kv_send.at[slot],
                recv_sem=kv_recv.at[slot],
                device_id={"kv": lax.rem(kv + step, n_kv)},
                device_id_type=MESH,
            )
            copy.start()
            copies.append(copy)
        sends.extend(copies)
        return copies

    load_resid.wait()
    pl.semaphore_wait(barrier, n_kv)
    swap = to_peer(0, halves.at[tp], halves.at[tp])
    load_gain1.wait()
    load_wq.wait()
    load_wk.wait()
    load_wv.wait()
    load_wf.wait()
    load_bias.wait()
    swap.wait_recv()

    offset = pl.multiple_of(kv * width, 128)
    lane = lax.broadcasted_iota(jnp.int32, (1, 128), 1)
    source = jnp.concatenate([halves[i].astype(F32) for i in range(n_tp)], axis=1)
    scaled = (source * gain1_v[:, pl.ds(offset, width)]).astype(BF16)
    squares = jnp.sum(source * source, axis=1, keepdims=True)
    proj[kv, :rows, : qw + 2 * kw] = jnp.dot(scaled, wqkv[...], preferred_element_type=F32)
    wf = wf_v[:, pl.ds(offset, width)].astype(F32)
    scaled32 = scaled.astype(F32)
    extra = jnp.broadcast_to(squares, (rows, 128))
    bias_rows = []
    for h in range(local_heads):
        picked = wf[h : h + 1]
        bias_h = bias_v[:, h : h + 1]
        for t in range(1, n_tp):
            g = t * local_heads + h
            picked = jnp.where(tp == t, wf[g : g + 1], picked)
            bias_h = jnp.where(tp == t, bias_v[:, g : g + 1], bias_h)
        bias_rows.append(bias_h)
        gate = jnp.sum(scaled32 * picked, axis=1, keepdims=True)
        extra = jnp.where(lane == h, gate, extra)
    proj[kv, :rows, qw + 2 * kw :] = extra

    copies = to_all(0, proj.at[kv])
    load_keys.wait()
    load_gates.wait()
    load_values.wait()
    for copy in copies:
        copy.wait_recv()
    total = proj[0, :rows, :]
    for i in range(1, n_kv):
        total = total + proj[i, :rows, :]
    extra = total[:, qw + 2 * kw :]
    inverse = lax.rsqrt(extra[:, local_heads : local_heads + 1] / features + EPS)
    query = (total[:, :qw] * inverse).astype(BF16).astype(F32) * (HEAD ** (-0.5))
    key_new = (total[:, qw : qw + kw] * inverse).astype(BF16).astype(F32)
    value_new = (total[:, qw + kw : qw + 2 * kw] * inverse).astype(BF16).astype(F32)
    low = lane < HEAD
    per_row = local_heads * group
    for t in range(group // 2):
        for h in range(local_heads):
            start = h * group * HEAD + t * 128
            block = query[:, start : start + 128]
            turned = pltpu.roll(block, HEAD, 1)
            first, second = (block, turned) if h == 0 else (turned, block)
            keep = low if h == 0 else jnp.logical_not(low)
            for j, item in ((2 * t, first), (2 * t + 1, second)):
                kept = jnp.where(keep, item, 0.0)
                for b in range(rows):
                    row = b * per_row + h * group + j
                    qs[row : row + 1, :] = kept[b : b + 1, :]
    forget = []
    for h in range(local_heads):
        z = extra[:, h : h + 1] * inverse + bias_rows[h]
        forget.append(jnp.minimum(z, 0.0) - jnp.log1p(jnp.exp(-jnp.abs(z))))

    def both(pair):
        return jnp.where(low, pair[:group], pair[group:])

    front = jnp.bitwise_and(lane, HEAD - 1) < HEAD // 2
    for b in range(rows):
        q_b = qs[b * per_row : (b + 1) * per_row, :].astype(BF16)
        scores = lax.dot_general(
            q_b, keys_v[b], (((1,), (1,)), ((), ())), preferred_element_type=F32
        )
        ctx = scores.shape[1]
        scores = scores + jnp.concatenate(
            [
                jnp.broadcast_to(gates_v[b, h : h + 1, :], (group, ctx))
                for h in range(local_heads)
            ],
            axis=0,
        )
        maxima = jnp.max(scores, axis=1, keepdims=True)
        weights = jnp.exp(scores - maxima)
        totals = jnp.sum(weights, axis=1, keepdims=True)
        mixed = jnp.dot(weights.astype(BF16), values_v[b], preferred_element_type=F32)
        peak = both(maxima) + jnp.where(low, forget[0][b : b + 1], forget[1][b : b + 1])
        soft[kv, 0, b * group : (b + 1) * group, :] = both(mixed)
        soft[kv, 1, b * group : (b + 1) * group, :] = jnp.where(front, peak, both(totals))
    copies = to_all(1, soft.at[kv])
    fresh, fresh_value = [], []
    for b in range(rows):
        q_b = qs[b * per_row : (b + 1) * per_row, :]
        fresh.append(both(jnp.sum(q_b * key_new[b : b + 1], axis=1, keepdims=True)))
        fresh_value.append(jnp.broadcast_to(value_new[b : b + 1], (group, 128)))
    fresh = jnp.concatenate(fresh, axis=0)
    fresh_value = jnp.concatenate(fresh_value, axis=0)
    for copy in copies:
        copy.wait_recv()
    peaks, counts = [], []
    for i in range(n_kv):
        stat = soft[i, 1]
        peaks.append(jnp.where(front, stat, pltpu.roll(stat, HEAD // 2, 1)))
        counts.append(jnp.where(front, pltpu.roll(stat, 128 - HEAD // 2, 1), stat))
    peak = fresh
    for item in peaks:
        peak = jnp.maximum(peak, item)
    own = jnp.exp(fresh - peak)
    count = own
    mixed = own.astype(BF16).astype(F32) * fresh_value
    for i in range(n_kv):
        scale = jnp.exp(peaks[i] - peak)
        count = count + counts[i] * scale
        mixed = mixed + soft[i, 0] * scale
    att[...] = mixed / count
    blocks = [[] for _ in range(local_heads)]
    for t in range(group // 2):
        pair = []
        for j in (2 * t, 2 * t + 1):
            pair.append(
                jnp.concatenate(
                    [att[b * group + j : b * group + j + 1, :] for b in range(rows)], axis=0
                )
            )
        blocks[0].append(jnp.where(low, pair[0], pltpu.roll(pair[1], HEAD, 1)))
        blocks[1].append(jnp.where(low, pltpu.roll(pair[0], HEAD, 1), pair[1]))
    attended = jnp.concatenate(blocks[0] + blocks[1], axis=1).astype(BF16)

    load_wo.wait()
    branch[tp, :rows, :] = jnp.dot(attended, wo_v[...], preferred_element_type=F32).astype(BF16)
    swap = to_peer(1, branch.at[tp], branch.at[tp])
    load_gain2.wait()
    load_wu.wait()
    swap.wait_recv()
    added = branch[0, :rows, :].astype(F32)
    for t in range(1, n_tp):
        added = added + branch[t, :rows, :].astype(F32)
    middle = (source + added).astype(BF16).astype(F32)
    scaled = (middle * gain2_v[:, pl.ds(offset, width)]).astype(BF16)
    squares = jnp.sum(middle * middle, axis=1, keepdims=True)
    norm2[kv, :rows, :] = jnp.broadcast_to(squares, (rows, 128))
    norm_copies = to_all(2, norm2.at[kv])
    up_copies = []
    for c in range(CHUNKS):
        ups[c, kv, :rows, :] = jnp.dot(
            scaled, wu_v[:, c * ff_chunk : (c + 1) * ff_chunk], preferred_element_type=F32
        ).astype(BF16)
        up_copies.append(to_all(3 + c, ups.at[c, kv]))
    load_wd.wait()
    for copy in norm_copies:
        copy.wait_recv()
    squares = norm2[0, :rows, :1]
    for i in range(1, n_kv):
        squares = squares + norm2[i, :rows, :1]
    inverse = lax.rsqrt(squares / features + EPS)
    down = jnp.zeros((rows, width), F32)
    for c in range(CHUNKS):
        for copy in up_copies[c]:
            copy.wait_recv()
        up = ups[c, 0, :rows, :].astype(F32)
        for i in range(1, n_kv):
            up = up + ups[c, i, :rows, :].astype(F32)
        hidden = jnp.square(jnp.maximum(up * inverse, 0.0)).astype(BF16)
        down = down + jnp.dot(
            hidden, wd_v[c * ff_chunk : (c + 1) * ff_chunk, :], preferred_element_type=F32
        )

    def part(value, which):
        picked = value[:, :half]
        for t in range(1, n_tp):
            picked = jnp.where(which == t, value[:, t * half : (t + 1) * half], picked)
        return picked

    tail_out[:rows, :] = part(down, peer).astype(BF16)
    swap = to_peer(2, tail_out, tail_in)
    kept = part(down, tp).astype(BF16).astype(F32)
    middle_half = part(middle, tp)
    swap.wait_recv()
    out[...] = (middle_half + (kept + tail_in[:rows, :].astype(F32))).astype(BF16)
    for copy in sends:
        copy.wait_send()


def layer(
    n_kv,
    n_tp,
    resid,
    keys_cache,
    values_cache,
    gates_cache,
    norm_gain,
    w_query,
    w_key,
    w_value,
    w_forget,
    forget_bias,
    w_out,
    mlp_gain,
    w_up,
    w_down,
):
    rows, half = resid.shape
    padded = -(-rows // 4) * 4
    width = half * n_tp
    qw, kw, ff = w_query.shape[1], w_key.shape[1], w_up.shape[1]
    group = HEADS // LOOKUP_GROUPS
    local_heads = kw // HEAD
    gates = jnp.transpose(gates_cache, (0, 2, 1))
    gain1, gain2 = norm_gain.reshape(1, -1), mlp_gain.reshape(1, -1)
    forget_t = jnp.transpose(w_forget)
    bias = forget_bias.reshape(1, -1)
    exchanges = 3 + CHUNKS
    return pl.pallas_call(
        functools.partial(layer_kernel, n_kv, n_tp),
        out_shape=jax.ShapeDtypeStruct((rows, half), BF16),
        in_specs=[pl.BlockSpec(memory_space=pl.ANY)] * 14,
        out_specs=pl.BlockSpec(memory_space=pltpu.VMEM),
        scratch_shapes=[
            pltpu.VMEM((n_tp, rows, half), BF16),
            pltpu.VMEM(gain1.shape, F32),
            pltpu.VMEM((w_query.shape[0], qw + 2 * kw), BF16),
            pltpu.VMEM(forget_t.shape, BF16),
            pltpu.VMEM(bias.shape, F32),
            pltpu.VMEM(keys_cache.shape, BF16),
            pltpu.VMEM(values_cache.shape, BF16),
            pltpu.VMEM(gates.shape, F32),
            pltpu.VMEM(w_out.shape, BF16),
            pltpu.VMEM(gain2.shape, F32),
            pltpu.VMEM(w_up.shape, BF16),
            pltpu.VMEM(w_down.shape, BF16),
            pltpu.VMEM((n_kv, padded, qw + 2 * kw + 128), F32),
            pltpu.VMEM((rows * local_heads * group, 128), F32),
            pltpu.VMEM((n_kv, 2, rows * group, 128), F32),
            pltpu.VMEM((rows * group, 128), F32),
            pltpu.VMEM((n_tp, padded, width), BF16),
            pltpu.VMEM((n_kv, padded, 128), F32),
            pltpu.VMEM((CHUNKS, n_kv, padded, ff // CHUNKS), BF16),
            pltpu.VMEM((padded, half), BF16),
            pltpu.VMEM((padded, half), BF16),
            pltpu.SemaphoreType.DMA((14,)),
            pltpu.SemaphoreType.DMA((3,)),
            pltpu.SemaphoreType.DMA((3,)),
            pltpu.SemaphoreType.DMA((exchanges * (n_kv - 1),)),
            pltpu.SemaphoreType.DMA((exchanges * (n_kv - 1),)),
        ],
        compiler_params=pltpu.CompilerParams(
            collective_id=0, has_side_effects=True, vmem_limit_bytes=60 * 1024 * 1024
        ),
    )(
        resid,
        keys_cache,
        values_cache,
        gates,
        gain1,
        w_query,
        w_key,
        w_value,
        forget_t,
        bias,
        w_out,
        gain2,
        w_up,
        w_down,
    )


def solution(mesh):
    in_specs = (
        P(("grp", "dp"), ("kv", "tp")),
        P(("grp", "dp"), "kv", "tp"),
        P(("grp", "dp"), "kv", "tp"),
        P(("grp", "dp"), "kv", "tp"),
        P(),
        P("kv", "tp"),
        P("kv", "tp"),
        P("kv", "tp"),
        P(),
        P(),
        P("tp", "kv"),
        P(),
        P("kv", "tp"),
        P("tp", "kv"),
    )
    body = functools.partial(layer, mesh.shape["kv"], mesh.shape["tp"])
    return jax.shard_map(
        body,
        mesh=mesh,
        in_specs=in_specs,
        out_specs=P(("grp", "dp"), ("kv", "tp")),
        check_vma=False,
    )
```

```python
import functools

import jax
import jax.numpy as jnp
from jax import lax
from jax.experimental import pallas as pl
from jax.experimental.pallas import tpu as pltpu
from jax.sharding import PartitionSpec as P

HEADS = 32
LOOKUP_GROUPS = 4
HEAD = 64
EPS = 1e-06
CHUNKS = 4
MESH = pl.DeviceIdType.MESH
F32 = jnp.float32
BF16 = jnp.bfloat16


def layer_kernel(
    n_kv,
    n_tp,
    resid,
    keys,
    values,
    gates,
    gain1,
    w_query,
    w_key,
    w_value,
    w_forget_t,
    bias,
    w_out,
    gain2,
    w_up,
    w_down,
    out,
    halves,
    gain1_v,
    wqkv,
    wf_v,
    bias_v,
    keys_v,
    values_v,
    gates_v,
    wo_v,
    gain2_v,
    wu_v,
    wd_v,
    proj,
    qs,
    soft,
    att,
    branch,
    norm2,
    ups,
    tail_out,
    tail_in,
    load_sem,
    tp_send,
    tp_recv,
    kv_send,
    kv_recv,
):
    kv = lax.axis_index("kv")
    tp = lax.axis_index("tp")
    peer = lax.rem(tp + 1, n_tp)
    rows, half = resid.shape
    width = half * n_tp
    features = width * n_kv
    qw = w_query.shape[1]
    kw = w_key.shape[1]
    local_heads = kw // HEAD
    group = HEADS // LOOKUP_GROUPS
    ff = w_up.shape[1]
    ff_chunk = ff // CHUNKS

    def load(index, source, target):
        copy = pltpu.make_async_copy(source, target, load_sem.at[index])
        copy.start()
        return copy

    load_resid = load(0, resid, halves.at[tp])
    load_gain1 = load(1, gain1, gain1_v)
    load_wq = load(2, w_query, wqkv.at[:, pl.ds(0, qw)])
    load_wk = load(3, w_key, wqkv.at[:, pl.ds(qw, kw)])
    load_wv = load(4, w_value, wqkv.at[:, pl.ds(qw + kw, kw)])
    load_wf = load(5, w_forget_t, wf_v)
    load_bias = load(6, bias, bias_v)

    barrier = pltpu.get_barrier_semaphore()
    pl.semaphore_signal(barrier, inc=1, device_id={"tp": peer}, device_id_type=MESH)
    for step in range(1, n_kv):
        pl.semaphore_signal(
            barrier, inc=1, device_id={"kv": lax.rem(kv + step, n_kv)}, device_id_type=MESH
        )
    load_keys = load(7, keys, keys_v)
    load_gates = load(8, gates, gates_v)
    load_values = load(9, values, values_v)
    load_wo = load(10, w_out, wo_v)
    load_gain2 = load(11, gain2, gain2_v)
    load_wu = load(12, w_up, wu_v)
    load_wd = load(13, w_down, wd_v)
    sends = []

    def to_peer(index, source, target):
        copy = pltpu.make_async_remote_copy(
            src_ref=source,
            dst_ref=target,
            send_sem=tp_send.at[index],
            recv_sem=tp_recv.at[index],
            device_id={"tp": peer},
            device_id_type=MESH,
        )
        copy.start()
        sends.append(copy)
        return copy

    def to_all(index, block):
        copies = []
        for step in range(1, n_kv):
            slot = index * (n_kv - 1) + step - 1
            copy = pltpu.make_async_remote_copy(
                src_ref=block,
                dst_ref=block,
                send_sem=kv_send.at[slot],
                recv_sem=kv_recv.at[slot],
                device_id={"kv": lax.rem(kv + step, n_kv)},
                device_id_type=MESH,
            )
            copy.start()
            copies.append(copy)
        sends.extend(copies)
        return copies

    load_resid.wait()
    pl.semaphore_wait(barrier, n_kv)
    swap = to_peer(0, halves.at[tp], halves.at[tp])
    lane = lax.broadcasted_iota(jnp.int32, (1, 128), 1)
    slot = jnp.bitwise_and(lane, HEAD - 1)

    def part(value, which):
        picked = value[:, :half]
        for t in range(1, n_tp):
            picked = jnp.where(which == t, value[:, t * half : (t + 1) * half], picked)
        return picked

    load_gain1.wait()
    load_wf.wait()
    load_bias.wait()
    offset = pl.multiple_of(kv * width, 128)
    gain = gain1_v[:, pl.ds(offset, width)]
    wf = wf_v[:, pl.ds(offset, width)].astype(F32)
    bias_rows, forget_rows = [], []
    for h in range(local_heads):
        picked = wf[h : h + 1]
        bias_h = bias_v[:, h : h + 1]
        for t in range(1, n_tp):
            g = t * local_heads + h
            picked = jnp.where(tp == t, wf[g : g + 1], picked)
            bias_h = jnp.where(tp == t, bias_v[:, g : g + 1], bias_h)
        bias_rows.append(bias_h)
        forget_rows.append(picked)

    def project(which):
        block = halves[which].astype(F32)
        scaled = (block * part(gain, which)).astype(BF16)
        start = pl.multiple_of(which * half, half)
        product = jnp.dot(scaled, wqkv[pl.ds(start, half), :], preferred_element_type=F32)
        extra = jnp.broadcast_to(jnp.sum(block * block, axis=1, keepdims=True), (rows, 128))
        for h in range(local_heads):
            gate = jnp.sum(
                scaled.astype(F32) * part(forget_rows[h], which), axis=1, keepdims=True
            )
            extra = jnp.where(slot == h, gate, extra)
        return product, extra

    load_wq.wait()
    load_wk.wait()
    load_wv.wait()
    product, extra = project(tp)
    swap.wait_recv()
    product_b, extra_b = project(peer)
    proj[kv, :rows, : qw + 2 * kw] = (product + product_b).astype(BF16)
    extra = extra + extra_b
    coarse = extra.astype(BF16).astype(F32)
    proj[kv, :rows, qw + 2 * kw :] = jnp.where(lane < HEAD, coarse, extra - coarse).astype(BF16)

    copies = to_all(0, proj.at[kv])
    load_keys.wait()
    load_gates.wait()
    load_values.wait()
    for copy in copies:
        copy.wait_recv()
    total = proj[0, :rows, :].astype(F32)
    for i in range(1, n_kv):
        total = total + proj[i, :rows, :].astype(F32)
    extra = total[:, qw + 2 * kw :]
    extra = extra + pltpu.roll(extra, HEAD, 1)
    inverse = lax.rsqrt(extra[:, local_heads : local_heads + 1] / features + EPS)
    query = (total[:, :qw] * inverse).astype(BF16).astype(F32) * (HEAD ** (-0.5))
    key_new = (total[:, qw : qw + kw] * inverse).astype(BF16).astype(F32)
    value_new = (total[:, qw + kw : qw + 2 * kw] * inverse).astype(BF16).astype(F32)
    low = lane < HEAD
    per_row = local_heads * group
    for t in range(group // 2):
        for h in range(local_heads):
            start = h * group * HEAD + t * 128
            block = query[:, start : start + 128]
            turned = pltpu.roll(block, HEAD, 1)
            first, second = (block, turned) if h == 0 else (turned, block)
            keep = low if h == 0 else jnp.logical_not(low)
            for j, item in ((2 * t, first), (2 * t + 1, second)):
                kept = jnp.where(keep, item, 0.0)
                for b in range(rows):
                    row = b * per_row + h * group + j
                    qs[row : row + 1, :] = kept[b : b + 1, :]
    forget = []
    for h in range(local_heads):
        z = extra[:, h : h + 1] * inverse + bias_rows[h]
        forget.append(jnp.minimum(z, 0.0) - jnp.log1p(jnp.exp(-jnp.abs(z))))

    def both(pair):
        return jnp.where(low, pair[:group], pair[group:])

    quarter = HEAD // 4
    front = slot < 2 * quarter
    even = jnp.bitwise_and(lane, 2 * quarter - 1) < quarter
    outcomes, stats = [], []

    def split(value):
        coarse = value.astype(BF16).astype(F32)
        return coarse, (value - coarse).astype(BF16).astype(F32)

    for b in range(rows):
        q_b = qs[b * per_row : (b + 1) * per_row, :].astype(BF16)
        scores = lax.dot_general(
            q_b, keys_v[b], (((1,), (1,)), ((), ())), preferred_element_type=F32
        )
        ctx = scores.shape[1]
        scores = scores + jnp.concatenate(
            [
                jnp.broadcast_to(gates_v[b, h : h + 1, :], (group, ctx))
                for h in range(local_heads)
            ],
            axis=0,
        )
        maxima = jnp.max(scores, axis=1, keepdims=True)
        high, low_part = split(maxima)
        weights = jnp.exp(scores - (high + low_part))
        totals = jnp.sum(weights, axis=1, keepdims=True)
        mixed = jnp.dot(weights.astype(BF16), values_v[b], preferred_element_type=F32)
        outcomes.append(both(mixed))
        count_high, count_low = split(totals)
        peak_tile = jnp.where(even, both(high), both(low_part))
        count_tile = jnp.where(even, both(count_high), both(count_low))
        stats.append(jnp.where(front, peak_tile, count_tile))
    soft[kv] = jnp.concatenate(outcomes + stats, axis=0).astype(BF16)
    copies = to_all(1, soft.at[kv])
    fresh, fresh_value = [], []
    for b in range(rows):
        q_b = qs[b * per_row : (b + 1) * per_row, :]
        own_score = both(jnp.sum(q_b * key_new[b : b + 1], axis=1, keepdims=True))
        own_gate = jnp.where(low, forget[0][b : b + 1], forget[1][b : b + 1])
        fresh.append(own_score - own_gate)
        fresh_value.append(jnp.broadcast_to(value_new[b : b + 1], (group, 128)))
    fresh = jnp.concatenate(fresh, axis=0)
    fresh_value = jnp.concatenate(fresh_value, axis=0)
    for copy in copies:
        copy.wait_recv()
    peaks, counts, partial = [], [], []
    cells = rows * group
    for i in range(n_kv):
        message = soft[i].astype(F32)
        partial.append(message[:cells])
        stat = message[cells:]
        stat = stat + jnp.where(
            even, pltpu.roll(stat, 128 - quarter, 1), pltpu.roll(stat, quarter, 1)
        )
        counts.append(stat)
        peaks.append(jnp.where(front, stat, pltpu.roll(stat, 2 * quarter, 1)))
    peak = fresh
    for item in peaks:
        peak = jnp.maximum(peak, item)
    own = jnp.exp(fresh - peak)
    count = 0.0
    mixed = own.astype(BF16).astype(F32) * fresh_value
    for i in range(n_kv):
        scale = jnp.exp(peaks[i] - peak)
        count = count + counts[i] * scale
        mixed = mixed + partial[i] * scale
    count = jnp.where(front, pltpu.roll(count, 128 - 2 * quarter, 1), count) + own
    att[...] = mixed / count
    blocks = [[] for _ in range(local_heads)]
    for t in range(group // 2):
        pair = []
        for j in (2 * t, 2 * t + 1):
            pair.append(
                jnp.concatenate(
                    [att[b * group + j : b * group + j + 1, :] for b in range(rows)], axis=0
                )
            )
        blocks[0].append(jnp.where(low, pair[0], pltpu.roll(pair[1], HEAD, 1)))
        blocks[1].append(jnp.where(low, pltpu.roll(pair[0], HEAD, 1), pair[1]))
    attended = jnp.concatenate(blocks[0] + blocks[1], axis=1).astype(BF16)

    load_wo.wait()
    branch[tp, :rows, :] = jnp.dot(attended, wo_v[...], preferred_element_type=F32).astype(BF16)
    swap = to_peer(1, branch.at[tp], branch.at[tp])
    load_gain2.wait()
    load_wu.wait()
    swap.wait_recv()
    source = jnp.concatenate([halves[t].astype(F32) for t in range(n_tp)], axis=1)
    added = branch[0, :rows, :].astype(F32)
    for t in range(1, n_tp):
        added = added + branch[t, :rows, :].astype(F32)
    middle = (source + added).astype(BF16).astype(F32)
    scaled = (middle * gain2_v[:, pl.ds(offset, width)]).astype(BF16)
    squares = jnp.sum(middle * middle, axis=1, keepdims=True)
    norm2[kv, :rows, :] = jnp.broadcast_to(squares, (rows, 128))
    norm_copies = to_all(2, norm2.at[kv])
    up_copies = []
    for c in range(CHUNKS):
        ups[c, kv, :rows, :] = jnp.dot(
            scaled, wu_v[:, c * ff_chunk : (c + 1) * ff_chunk], preferred_element_type=F32
        ).astype(BF16)
        up_copies.append(to_all(3 + c, ups.at[c, kv]))
    load_wd.wait()
    for copy in norm_copies:
        copy.wait_recv()
    squares = norm2[0, :rows, :1]
    for i in range(1, n_kv):
        squares = squares + norm2[i, :rows, :1]
    inverse = lax.rsqrt(squares / features + EPS)
    down = jnp.zeros((rows, width), F32)
    for c in range(CHUNKS):
        for copy in up_copies[c]:
            copy.wait_recv()
        up = ups[c, 0, :rows, :].astype(F32)
        for i in range(1, n_kv):
            up = up + ups[c, i, :rows, :].astype(F32)
        hidden = jnp.square(jnp.maximum(up * inverse, 0.0)).astype(BF16)
        down = down + jnp.dot(
            hidden, wd_v[c * ff_chunk : (c + 1) * ff_chunk, :], preferred_element_type=F32
        )

    tail_out[:rows, :] = part(down, peer).astype(BF16)
    swap = to_peer(2, tail_out, tail_in)
    kept = part(down, tp).astype(BF16).astype(F32)
    middle_half = part(middle, tp)
    swap.wait_recv()
    out[...] = (middle_half + (kept + tail_in[:rows, :].astype(F32))).astype(BF16)
    for copy in sends:
        copy.wait_send()


def layer(
    n_kv,
    n_tp,
    resid,
    keys_cache,
    values_cache,
    gates_cache,
    norm_gain,
    w_query,
    w_key,
    w_value,
    w_forget,
    forget_bias,
    w_out,
    mlp_gain,
    w_up,
    w_down,
):
    rows, half = resid.shape
    padded = -(-rows // 4) * 4
    width = half * n_tp
    qw, kw, ff = w_query.shape[1], w_key.shape[1], w_up.shape[1]
    group = HEADS // LOOKUP_GROUPS
    local_heads = kw // HEAD
    gates = jnp.transpose(gates_cache, (0, 2, 1))
    gain1, gain2 = norm_gain.reshape(1, -1), mlp_gain.reshape(1, -1)
    forget_t = jnp.transpose(w_forget)
    bias = forget_bias.reshape(1, -1)
    exchanges = 3 + CHUNKS
    return pl.pallas_call(
        functools.partial(layer_kernel, n_kv, n_tp),
        out_shape=pltpu.VMEM((rows, half), BF16),
        in_specs=[pl.BlockSpec(memory_space=pl.ANY)] * 14,
        out_specs=pl.BlockSpec(memory_space=pltpu.VMEM),
        scratch_shapes=[
            pltpu.VMEM((n_tp, rows, half), BF16),
            pltpu.VMEM(gain1.shape, F32),
            pltpu.VMEM((w_query.shape[0], qw + 2 * kw), BF16),
            pltpu.VMEM(forget_t.shape, BF16),
            pltpu.VMEM(bias.shape, F32),
            pltpu.VMEM(keys_cache.shape, BF16),
            pltpu.VMEM(values_cache.shape, BF16),
            pltpu.VMEM(gates.shape, F32),
            pltpu.VMEM(w_out.shape, BF16),
            pltpu.VMEM(gain2.shape, F32),
            pltpu.VMEM(w_up.shape, BF16),
            pltpu.VMEM(w_down.shape, BF16),
            pltpu.VMEM((n_kv, padded, qw + 2 * kw + 128), BF16),
            pltpu.VMEM((rows * local_heads * group, 128), F32),
            pltpu.VMEM((n_kv, 2 * rows * group, 128), BF16),
            pltpu.VMEM((rows * group, 128), F32),
            pltpu.VMEM((n_tp, padded, width), BF16),
            pltpu.VMEM((n_kv, padded, 128), F32),
            pltpu.VMEM((CHUNKS, n_kv, padded, ff // CHUNKS), BF16),
            pltpu.VMEM((padded, half), BF16),
            pltpu.VMEM((padded, half), BF16),
            pltpu.SemaphoreType.DMA((14,)),
            pltpu.SemaphoreType.DMA((3,)),
            pltpu.SemaphoreType.DMA((3,)),
            pltpu.SemaphoreType.DMA((exchanges * (n_kv - 1),)),
            pltpu.SemaphoreType.DMA((exchanges * (n_kv - 1),)),
        ],
        compiler_params=pltpu.CompilerParams(
            collective_id=0, has_side_effects=True, vmem_limit_bytes=60 * 1024 * 1024
        ),
    )(
        resid,
        keys_cache,
        values_cache,
        gates,
        gain1,
        w_query,
        w_key,
        w_value,
        forget_t,
        bias,
        w_out,
        gain2,
        w_up,
        w_down,
    )


def solution(mesh):
    in_specs = (
        P(("grp", "dp"), ("kv", "tp")),
        P(("grp", "dp"), "kv", "tp"),
        P(("grp", "dp"), "kv", "tp"),
        P(("grp", "dp"), "kv", "tp"),
        P(),
        P("kv", "tp"),
        P("kv", "tp"),
        P("kv", "tp"),
        P(),
        P(),
        P("tp", "kv"),
        P(),
        P("kv", "tp"),
        P("tp", "kv"),
    )
    body = functools.partial(layer, mesh.shape["kv"], mesh.shape["tp"])
    return jax.shard_map(
        body,
        mesh=mesh,
        in_specs=in_specs,
        out_specs=P(("grp", "dp"), ("kv", "tp")),
        check_vma=False,
    )
```
